512 devices in a mesh: sp: 128 (over z, x, core), tp: 4 (over y).
Axes of the slice: x: 4, y: 4, z: 16, core: 2. Of those that a mesh axis runs over, the one named last changes fastest.
Arguments:
- tokens: bfloat16 [81920, 2048], P(('sp', 'tp')), may hold values from -44 to 44
- in_gain: float32 [2048], replicated, may hold values from 0.1 to 1.9
- w_x: bfloat16 [2048, 2048], P('sp', 'tp'), may hold values from -0.125 to 0.125
- w_z: bfloat16 [2048, 2048], P('sp', 'tp'), may hold values from -0.125 to 0.125
- w_b: bfloat16 [2048, 1024], P('sp', 'tp'), may hold values from -0.125 to 0.125
- w_c: bfloat16 [2048, 1024], P('sp', 'tp'), may hold values from -0.125 to 0.125
- w_dt: bfloat16 [2048, 32], replicated, may hold values from -0.125 to 0.125
- conv_x: float32 [4, 2048], replicated, may hold values from -3 to 3
- conv_b: float32 [4, 1024], replicated, may hold values from -3 to 3
- conv_c: float32 [4, 1024], replicated, may hold values from -3 to 3
- dt_bias: float32 [32], replicated, may hold values from -15 to -3.5
- a_log: float32 [32], replicated, may hold values from -0.5 to 0.5
- out_gain: float32 [2048], replicated, may hold values from 0.1 to 1.9
- w_out: bfloat16 [2048, 2048], P('tp', 'sp'), may hold values from -0.125 to 0.125
Outputs:
- mixer_out: bfloat16 [81920, 2048], P(('sp', 'tp'))
The draws below stay inside these ranges and needn't reach their ends.
All inputs are finite; a program needn't handle non-finite values.
Results may differ from the reference program's by a relative error of at most 0.015.
Values may be sent and summed in bfloat16 or wider, within the bound.
No kernel may reach another device: no remote copies, remote signals or barrier semaphores. Data moves between devices by JAX's collectives and lax.ppermute only.
A program may use at most 128 MiB of HBM per device.

```python
import math
import jax
import jax.numpy as jnp
from jax import lax

D = 2048
HEADS = 32
GROUPS = 8
HEAD_DIM = 64
STATE = 128
CONV = 4
BLOCK = 128
SEG = 640
INNER = 2048
LENGTH = 81920
N_TP = 4


def draw_tokens(key, part):
    base_key, lift_key, axis_key = jax.random.split(key, 3)
    segments = LENGTH // SEG
    base_rows = jnp.clip(jax.random.normal(base_key, (segments, SEG, D), jnp.float32), -6.0, 6.0)
    block_lift = jax.random.uniform(lift_key, (segments, 1, 1), jnp.float32, -1.2, 1.2)
    direction = jnp.clip(jax.random.normal(axis_key, (1, 1, D), jnp.float32), -4.0, 4.0)
    values = (base_rows + block_lift * direction).reshape(LENGTH, D)
    return values.astype(jnp.bfloat16)


def draw_dt_bias(key, part):
    pick_key, jitter_key = jax.random.split(key)
    slow_share = 0.5
    slow_heads = jax.random.uniform(pick_key, (HEADS,), jnp.float32) < slow_share
    jitter = jax.random.uniform(jitter_key, (HEADS,), jnp.float32, -0.5, 0.5)
    slow_value = -math.log(LENGTH) - 0.3 + jitter
    fast_value = -4.0 + jitter
    return jnp.where(slow_heads, slow_value, fast_value).astype(jnp.float32)


def block_scale(rng, shape, cuts, smallest, high):
    loudness = 1.0
    for position, shards_of in cuts:
        steps = jax.random.uniform(jax.random.fold_in(jax.random.fold_in(rng, 6), position), (shards_of,), jnp.float32, smallest / len(cuts), high / len(cuts))
        loudness = loudness * jnp.repeat(jnp.exp(steps), shape[position] // shards_of).reshape((-1,) + (1,) * (len(shape) - 1 - position))
    return loudness


def normal_values(key, shape, deviation, bound, shards=(), kind=jnp.bfloat16):
    drawn = jax.random.normal(key, shape, jnp.float32) * deviation
    if len(shards) > 0:
        drawn = block_scale(key, shape, shards, -0.22, 0.18) * drawn
    return jnp.clip(drawn, min=-bound, max=bound).astype(kind)


def setup_inputs(seed: int = 0) -> dict:
    key_of = jax.random.split(jax.random.key(seed), 15)
    return {
        "tokens": draw_tokens(jax.random.fold_in(key_of[14], 71), 0),
        "in_gain": jnp.clip(1.0 + 0.18 * jax.random.normal(key_of[1], (D,), jnp.float32), 0.1, 1.9),
        "w_x": normal_values(key_of[2], (D, INNER), D ** -0.5, 0.125, ((0, 128), (1, 4))),
        "w_z": normal_values(key_of[3], (D, INNER), D ** -0.5, 0.125, ((0, 128), (1, 4))),
        "w_b": normal_values(key_of[4], (D, GROUPS * STATE), D ** -0.5, 0.125, ((0, 128), (1, 4))),
        "w_c": normal_values(key_of[5], (D, GROUPS * STATE), D ** -0.5, 0.125, ((0, 128), (1, 4))),
        "w_dt": normal_values(key_of[6], (D, HEADS), D ** -0.5, 0.125),
        "conv_x": normal_values(key_of[7], (CONV, INNER), CONV ** -0.5, 3.0, (), jnp.float32),
        "conv_b": normal_values(key_of[8], (CONV, GROUPS * STATE), CONV ** -0.5, 3.0, (), jnp.float32),
        "conv_c": normal_values(key_of[9], (CONV, GROUPS * STATE), CONV ** -0.5, 3.0, (), jnp.float32),
        "dt_bias": draw_dt_bias(jax.random.fold_in(key_of[14], 71), 0),
        "a_log": jnp.clip(jax.random.uniform(key_of[11], (HEADS,), jnp.float32, -0.5, 0.5), -0.5, 0.5),
        "out_gain": jnp.clip(1.0 + 0.18 * jax.random.normal(key_of[12], (INNER,), jnp.float32), 0.1, 1.9),
        "w_out": normal_values(key_of[13], (INNER, D), INNER ** -0.5, 0.125, ((0, 4), (1, 128))),
    }


EPS = 1e-06
HIGH = lax.Precision.HIGHEST

def inverse_rms(values):
    return lax.rsqrt(lax.optimization_barrier(jnp.mean(values * values, axis=-1, keepdims=True)) + EPS)

def causal_conv(prev_rows, new_rows, kernel):
    joined = jnp.concatenate([prev_rows, new_rows], axis=0).astype(jnp.float32)
    row_count = new_rows.shape[0]
    summed = jnp.zeros(new_rows.shape, jnp.float32)
    for offset in range(CONV):
        summed = summed + kernel[offset] * joined[offset:offset + row_count]
    return jax.nn.silu(summed)

def project(normed, weight):
    return jnp.dot(normed.astype(jnp.float32), weight, precision=HIGH, preferred_element_type=jnp.float32)

def reference(tokens, in_gain, w_x, w_z, w_b, w_c, w_dt, conv_x, conv_b, conv_c, dt_bias, a_log, out_gain, w_out):
    group_heads = HEADS // GROUPS
    share_width = INNER // N_TP
    conv_keep = CONV - 1
    weights_in = tuple((weight.astype(jnp.float32) for weight in (w_x, w_z, w_b, w_c, w_dt)))
    weight_out = w_out.astype(jnp.float32)
    decay_rates = jnp.exp(a_log)
    causal = lax.broadcasted_iota(jnp.int32, (BLOCK, BLOCK), 0) >= lax.broadcasted_iota(jnp.int32, (BLOCK, BLOCK), 1)
    lower_ones = causal.astype(jnp.float32)

    def advance(carried_in, block_rows):
        run_state, prev_x, prev_b, prev_c = carried_in
        values = block_rows.astype(jnp.float32)
        normed = (values * inverse_rms(values) * in_gain).astype(jnp.bfloat16)
        proj_x, proj_z, proj_b, proj_c = [project(normed, weight).astype(jnp.bfloat16) for weight in weights_in[:4]]
        dt_raw = project(normed, weights_in[4])
        conv_xs = causal_conv(prev_x, proj_x, conv_x)
        conv_bs = causal_conv(prev_b, proj_b, conv_b)
        conv_cs = causal_conv(prev_c, proj_c, conv_c)
        step_size = jax.nn.softplus(dt_raw + dt_bias)
        log_decay = -step_size * decay_rates
        cum_decay = jnp.dot(lower_ones, log_decay, precision=HIGH)
        scaled_x = conv_xs.reshape(BLOCK, HEADS, HEAD_DIM) * step_size[:, :, None]
        b_heads = jnp.repeat(conv_bs.reshape(BLOCK, GROUPS, STATE), group_heads, axis=1)
        c_heads = jnp.repeat(conv_cs.reshape(BLOCK, GROUPS, STATE), group_heads, axis=1)
        scores = jnp.einsum('lhn,shn->hls', c_heads, b_heads, precision=HIGH)
        decay_gap = cum_decay.T[:, :, None] - cum_decay.T[:, None, :]
        within = jnp.where(causal, jnp.exp(jnp.where(causal, decay_gap, 0.0)), 0.0) * scores
        inside = jnp.einsum('hls,shp->lhp', within, scaled_x, precision=HIGH)
        carried = jnp.einsum('lhn,hpn->lhp', c_heads, run_state, precision=HIGH) * jnp.exp(cum_decay)[:, :, None]
        block_total = cum_decay[BLOCK - 1]
        tail_weight = jnp.exp(block_total[None, :] - cum_decay)
        new_state = run_state * jnp.exp(block_total)[:, None, None] + jnp.einsum('lhp,lhn->hpn', scaled_x * tail_weight[:, :, None], b_heads, precision=HIGH)
        gated_out = (inside + carried).reshape(BLOCK, INNER) * jax.nn.silu(proj_z.astype(jnp.float32))
        grouped = gated_out.reshape(BLOCK, GROUPS, INNER // GROUPS)
        mixed_rows = ((grouped * inverse_rms(grouped)).reshape(BLOCK, INNER) * out_gain).astype(jnp.bfloat16)
        summed = jnp.zeros((BLOCK, D), jnp.float32)
        for share_index in range(N_TP):
            columns = mixed_rows[:, share_index * share_width:(share_index + 1) * share_width]
            partial_sum = project(columns, weight_out[share_index * share_width:(share_index + 1) * share_width]).astype(jnp.bfloat16)
            summed = summed + lax.optimization_barrier(partial_sum).astype(jnp.float32)
        new_carry = (new_state, proj_x[BLOCK - conv_keep:], proj_b[BLOCK - conv_keep:], proj_c[BLOCK - conv_keep:])
        return (new_carry, summed.astype(jnp.bfloat16))
    initial = (jnp.zeros((HEADS, HEAD_DIM, STATE), jnp.float32), jnp.zeros((conv_keep, INNER), jnp.bfloat16), jnp.zeros((conv_keep, GROUPS * STATE), jnp.bfloat16), jnp.zeros((conv_keep, GROUPS * STATE), jnp.bfloat16))
    unused, outputs = lax.scan(advance, initial, tokens.reshape(LENGTH // BLOCK, BLOCK, D))
    return outputs.reshape(LENGTH, D)
```

```python
import jax
import jax.numpy as jnp
from jax import lax
from jax.experimental import pallas as pl
from jax.experimental.pallas import tpu as pltpu
from jax.sharding import Mesh
from jax.sharding import PartitionSpec as P

HEAD_DIM = 64
STATE = 128
CONV = 4
BLOCK = 128
EPS = 1e-06
F32 = jnp.float32
BF16 = jnp.bfloat16
ALL = ("z", "x", "c", "y")

SMEM = pl.BlockSpec(memory_space=pltpu.SMEM)
VMEM = pl.BlockSpec(memory_space=pltpu.VMEM)


def cycle(count, step):
    return [(a, (a + step) % count) for a in range(count)]


def silu(v):
    return v / (1.0 + jnp.exp(-v))


def local_call(kernel, outs, ins, scalars=0, scratch=(), mib=16):
    return pl.pallas_call(
        kernel,
        out_shape=outs,
        in_specs=[SMEM] * scalars + [VMEM] * (len(ins) - scalars),
        out_specs=jax.tree.map(lambda _: VMEM, outs),
        scratch_shapes=list(scratch),
        compiler_params=pltpu.CompilerParams(vmem_limit_bytes=mib << 20),
    )(*ins)


def to_all(value, axis, copies):
    return lax.all_to_all(
        jnp.broadcast_to(value, (copies, *value.shape)), axis, 0, 0, tiled=True
    )


def rotate_kernel(at, *refs):
    *pieces, out = refs
    count = len(pieces)
    for k in range(count):
        slot = lax.rem(at[0] + count - k, count)
        out[:, pl.ds(slot, 1)] = pieces[k][...][:, None]


def placed(pieces, at):
    lead, *rest = pieces[0].shape
    out = jax.ShapeDtypeStruct((lead, len(pieces), *rest), pieces[0].dtype)
    return local_call(rotate_kernel, out, (at, *pieces), 1, mib=8)


def around(value, axis):
    count = lax.axis_size(axis)
    return [value] + [lax.ppermute(value, axis, cycle(count, k)) for k in range(1, count)]


def norm_kernel(at, gain, tail, *refs):
    *pieces, out = refs
    count = len(pieces)
    rows = pieces[0].shape[0]

    def normed(values):
        values = values.astype(F32)
        mean = jnp.mean(values * values, axis=-1, keepdims=True)
        return (values * lax.rsqrt(mean + EPS) * gain[...]).astype(BF16)

    out[count * rows :, :] = normed(tail[...])
    for k in range(count):
        first = lax.rem(at[0] + count - k, count) * rows

        def chunk(r, carry):
            to = pl.multiple_of(first + r * 16, 16)
            out[pl.ds(to, 16), :] = normed(pieces[k][pl.ds(pl.multiple_of(r * 16, 16), 16), :])
            return carry

        lax.fori_loop(0, rows // 16, chunk, 0, unroll=5)


def scan_kernel(
    core, own, other, step, rate, taps, y_out, c_out, reach_out, state_out, rows_seq, buf, state, offset
):
    length = step.shape[0]
    inner = y_out.shape[1] // 2
    heads = inner // HEAD_DIM
    rows_seq[pl.ds(core[0], 1)] = own[...][None]
    rows_seq[pl.ds(1 - core[0], 1)] = other[...][None]
    buf[:, 0:8, :] = rows_seq[:, length + 8 : length + 16, :].astype(F32)
    state[...] = jnp.zeros_like(state)
    offset[...] = jnp.zeros_like(offset)
    causal = lax.broadcasted_iota(jnp.int32, (BLOCK, BLOCK), 0) >= lax.broadcasted_iota(
        jnp.int32, (BLOCK, BLOCK), 1
    )
    lower = causal.astype(F32)

    def block(i, carry):
        here = pl.ds(i * BLOCK, BLOCK)
        steps = step[here, :]
        cum = jnp.dot(
            lower, -steps * rate[...], precision=lax.Precision.HIGHEST, preferred_element_type=F32
        )
        cum_t = cum.T
        total = cum[BLOCK - 1 : BLOCK, :]
        decay = jnp.exp(cum)
        tail_weight = jnp.exp(total - cum)
        total_decay = jnp.exp(total)
        reach_out[here, :] = jnp.exp(cum + offset[...])
        offset[...] = offset[...] + total
        for g in range(2):
            buf[g, 8 : 8 + BLOCK, :] = rows_seq[g, here, :].astype(F32)
            summed = taps[g, 0:1, :] * buf[g, 5 : 5 + BLOCK, :]
            for k in range(1, CONV):
                summed = summed + taps[g, k : k + 1, :] * buf[g, 5 + k : 5 + k + BLOCK, :]
            buf[g, 0:8, :] = buf[g, BLOCK : BLOCK + 8, :]
            mixed = silu(summed)
            xs = mixed[:, :inner]
            bs = mixed[:, inner : inner + STATE]
            cs = mixed[:, inner + STATE :].astype(BF16)
            scores = lax.dot_general(
                cs, bs.astype(BF16), (((1,), (1,)), ((), ())), preferred_element_type=F32
            )
            old = state[g]
            reached = jnp.dot(cs, old.astype(BF16), preferred_element_type=F32)
            tails, factors, ys = [], [], []
            for h in range(heads):
                cut = slice(h * HEAD_DIM, (h + 1) * HEAD_DIM)
                lane = slice(g * heads + h, g * heads + h + 1)
                scaled = xs[:, cut] * steps[:, lane]
                gap = cum[:, lane] - cum_t[lane, :]
                within = jnp.where(causal, jnp.exp(jnp.where(causal, gap, 0.0)), 0.0) * scores
                inside = jnp.dot(
                    within.astype(BF16), scaled.astype(BF16), preferred_element_type=F32
                )
                ys.append(inside + reached[:, cut] * decay[:, lane])
                tails.append(scaled * tail_weight[:, lane])
                factors.append(jnp.broadcast_to(total_decay[:, lane], (1, HEAD_DIM)))
            y_out[here, g * inner : (g + 1) * inner] = jnp.concatenate(ys, axis=1)
            c_out[here, g * STATE : (g + 1) * STATE] = cs
            fresh = jnp.dot(
                bs.T.astype(BF16),
                jnp.concatenate(tails, axis=1).astype(BF16),
                preferred_element_type=F32,
            )
            state[g] = old * jnp.concatenate(factors, axis=1) + fresh
        return carry

    lax.fori_loop(0, length // BLOCK, block, 0)
    share = STATE // state_out.shape[0]
    for part in range(state_out.shape[0]):
        rows = slice(part * share, (part + 1) * share)
        write_packed(
            state_out,
            part,
            jnp.concatenate([state[0, rows, :], state[1, rows, :]], axis=1),
            jnp.exp(offset[...]),
        )


def write_packed(out, part, states, factor):
    width = states.shape[1]
    high = factor.astype(BF16).astype(F32)
    low = factor - high
    pick = lax.broadcasted_iota(jnp.int32, (states.shape[0], factor.shape[1]), 0)
    extra = jnp.where(pick == 0, high, jnp.where(pick == 1, low, 0.0))
    out[part, :, 0:width] = states.astype(BF16)
    out[part, :, width:] = extra.astype(BF16)


def read_packed(ref, part):
    width = ref.shape[2] - 128
    extra = ref[part, :, width:].astype(F32)
    return extra[0:1, :] + extra[1:2, :], ref[part, :, 0:width].astype(F32)


def widened(factor, width):
    return jnp.concatenate(
        [
            jnp.broadcast_to(factor[:, h : h + 1], (factor.shape[0], HEAD_DIM))
            for h in range(width // HEAD_DIM)
        ],
        axis=1,
    )


def plane_kernel(pieces, out):
    factor, states = read_packed(pieces, 0)
    for k in range(1, pieces.shape[0]):
        next_factor, next_states = read_packed(pieces, k)
        states = states * widened(next_factor, states.shape[1]) + next_states
        factor = factor * next_factor
    for k in range(out.shape[0]):
        write_packed(out, k, states, factor)


def enter_kernel(at, pieces, planes, out):
    run = jnp.zeros(out.shape[1:], F32)
    for k in range(planes.shape[0]):
        factor, states = read_packed(planes, k)
        run = jnp.where(k < at[0], run * widened(factor, run.shape[1]) + states, run)
    for k in range(pieces.shape[0]):
        out[k] = run.astype(BF16)
        factor, states = read_packed(pieces, k)
        run = run * widened(factor, run.shape[1]) + states


def gate_kernel(core, y, cs, reach, entering, gate_own, gate_other, gain, out):
    inner = y.shape[1] // 2
    heads = inner // HEAD_DIM

    def block(i, carry):
        here = pl.ds(pl.multiple_of(i * BLOCK, BLOCK), BLOCK)
        weight = reach[here, :]
        own, other = (gate[here, :].astype(F32) for gate in (gate_own, gate_other))
        for g in range(2):
            cut = slice(g * inner, (g + 1) * inner)
            reached = jnp.dot(
                cs[here, g * STATE : (g + 1) * STATE],
                entering[:, cut],
                preferred_element_type=F32,
            )
            expanded = widened(weight[:, g * heads : (g + 1) * heads], inner)
            gates = jnp.where(core[0] == g, own, other)
            gated = (y[here, cut] + reached * expanded) * silu(gates)
            mean = jnp.mean(gated * gated, axis=-1, keepdims=True)
            out[here, cut] = (gated * lax.rsqrt(mean + EPS) * gain[:, cut]).astype(BF16)
        return carry

    lax.fori_loop(0, y.shape[0] // BLOCK, block, 0)


def dot(a, b):
    return jnp.dot(a, b, preferred_element_type=F32)


def dot_t(a, b):
    return lax.dot_general(a, b, (((1,), (1,)), ((), ())), preferred_element_type=F32)


def body(
    tokens, in_gain, w_x, w_z, w_b, w_c, w_dt, conv_x, conv_b, conv_c, dt_bias, a_log, out_gain, w_out
):
    x_at, c_at, y_at, z_at = (lax.axis_index(a) for a in ("x", "c", "y", "z"))
    x_one, c_one, y_one, z_one = (v.reshape(1) for v in (x_at, c_at, y_at, z_at))
    n_z, n_x, n_y = (lax.axis_size(a) for a in ("z", "x", "y"))
    rows, width = tokens.shape
    length = rows * n_y
    inner = w_x.shape[1] // 2
    state = w_b.shape[1] // 2
    heads = 2 * inner // HEAD_DIM
    cut = inner + 2 * state
    core_swap = cycle(2, 1)

    def halves_swapped(*arrays):
        def columns_of(core):
            return jnp.concatenate(
                [
                    lax.dynamic_slice_in_dim(w, core * (w.shape[1] // 2), w.shape[1] // 2, 1)
                    for w in arrays
                ],
                axis=1,
            )

        mine = columns_of(c_at)
        swapped = lax.ppermute(columns_of(1 - c_at), "c", core_swap)
        return jnp.where(
            c_at == 0,
            jnp.concatenate([mine, swapped], axis=0),
            jnp.concatenate([swapped, mine], axis=0),
        )

    first_source = halves_swapped(w_x, w_b, w_c)
    pieces = around(tokens, "y")
    first_z = to_all(first_source, "z", n_z)
    first_pieces = around(first_z, "x")
    second_source = halves_swapped(w_z, w_out.T)
    second_source, first_z = lax.optimization_barrier((second_source, first_z))
    second_z = to_all(second_source, "z", n_z)

    ends = lax.select_n(lax.rem(y_at + 1, n_y), *(piece[rows - 16 :] for piece in pieces))
    chain_steps = [(a, a + 1) for a in range(2 * n_z * n_x - 1)]
    tail = lax.ppermute(ends, ("z", "x", "c"), chain_steps)
    normed = local_call(
        norm_kernel,
        jax.ShapeDtypeStruct((length + 16, width), BF16),
        (y_one, in_gain.reshape(1, -1), tail, *pieces),
        1,
    )

    def here(v, size):
        return lax.dynamic_slice_in_dim(v, y_at * size, size, v.ndim - 1)

    lanes = 128
    dt_weight = jnp.pad(here(w_dt, heads), ((0, 0), (0, lanes - heads)))
    bias = jnp.pad(here(dt_bias, heads), (0, lanes - heads))
    rate = jnp.pad(jnp.exp(here(a_log, heads)), (0, lanes - heads)).reshape(1, lanes)
    step = jax.nn.softplus(dot(normed[:length], dt_weight) + bias)
    taps = jnp.concatenate(
        [
            here(v, 2 * size).reshape(CONV, 2, size).swapaxes(0, 1)
            for v, size in ((conv_x, inner), (conv_b, state), (conv_c, state))
        ],
        axis=2,
    )

    first_pieces, step = lax.optimization_barrier((first_pieces, step))
    first = placed(first_pieces, x_one).reshape(width, cut)
    first_other = lax.ppermute(first, "c", core_swap)
    second_pieces = around(second_z, "x")
    second = placed(second_pieces, x_one).reshape(width, 2 * inner)
    second_other = lax.ppermute(second, "c", core_swap)

    proj = [dot(normed, w).astype(BF16) for w in (first, first_other)]
    parts = 2 * n_x
    share = STATE // parts
    y_local, c_rows, reach, final = local_call(
        scan_kernel,
        (
            jax.ShapeDtypeStruct((length, 2 * inner), F32),
            jax.ShapeDtypeStruct((length, 2 * STATE), BF16),
            jax.ShapeDtypeStruct((length, lanes), F32),
            jax.ShapeDtypeStruct((parts, share, 2 * inner + lanes), BF16),
        ),
        (c_one, *proj, step, rate, taps),
        1,
        (
            pltpu.VMEM((2, length + 16, cut), BF16),
            pltpu.VMEM((2, BLOCK + 8, cut), F32),
            pltpu.VMEM((2, STATE, inner), F32),
            pltpu.VMEM((1, lanes), F32),
        ),
    )

    within_plane = lax.all_to_all(final, ("x", "c"), 0, 0, tiled=True)
    sent = local_call(
        plane_kernel, jax.ShapeDtypeStruct((n_z, share, 2 * inner + lanes), BF16), (within_plane,)
    )
    planes = lax.all_to_all(sent, "z", 0, 0, tiled=True)
    back = local_call(
        enter_kernel,
        jax.ShapeDtypeStruct((parts, share, 2 * inner), BF16),
        (z_one, within_plane, planes),
        1,
    )
    entering = lax.all_to_all(back, ("x", "c"), 0, 0, tiled=True).reshape(STATE, 2 * inner)

    gates = [dot(normed[:length], w[:, :inner]).astype(BF16) for w in (second, second_other)]
    halves = [w[:, inner:] for w in (second, second_other)]
    out_weight = jnp.where(
        c_at == 0, jnp.concatenate(halves, axis=1), jnp.concatenate(halves[::-1], axis=1)
    )
    mixed = local_call(
        gate_kernel,
        jax.ShapeDtypeStruct((length, 2 * inner), BF16),
        (c_one, y_local, c_rows, reach, entering, *gates, here(out_gain, 2 * inner).reshape(1, -1)),
        1,
    ).reshape(n_y, rows, 2 * inner)

    def partial(k):
        share_rows = lax.dynamic_index_in_dim(mixed, lax.rem(y_at + k, n_y), 0, keepdims=False)
        return dot_t(share_rows, out_weight).astype(BF16)

    received = [lax.ppermute(partial(k), "y", cycle(n_y, k)) for k in (2, 1, 3)]
    summed = partial(0).astype(F32)
    for piece in received:
        summed = summed + piece.astype(F32)
    return summed.astype(BF16)


def solution(mesh):
    split = Mesh(mesh.devices.reshape(16, 4, 2, mesh.shape["tp"]), ALL)
    sp = ("z", "x", "c")
    in_specs = (
        P(ALL, None), P(), P(sp, "y"), P(sp, "y"), P(sp, "y"), P(sp, "y"),
        P(), P(), P(), P(), P(), P(), P(), P("y", sp),
    )
    return jax.shard_map(
        body, mesh=split, in_specs=in_specs, out_specs=P(ALL, None), check_vma=False
    )
```

```python
import jax
import jax.numpy as jnp
from jax import lax
from jax.experimental import pallas as pl
from jax.experimental.pallas import tpu as pltpu
from jax.sharding import Mesh
from jax.sharding import PartitionSpec as P

HEAD_DIM = 64
STATE = 128
CONV = 4
BLOCK = 128
EPS = 1e-06
F32 = jnp.float32
BF16 = jnp.bfloat16
ALL = ("z", "x", "c", "y")


SMEM = pl.BlockSpec(memory_space=pltpu.SMEM)
VMEM = pl.BlockSpec(memory_space=pltpu.VMEM)


def cycle(count, step):
    return [(a, (a + step) % count) for a in range(count)]


def silu(v):
    return v / (1.0 + jnp.exp(-v))


def local_call(kernel, outs, ins, scalars=0, scratch=(), mib=16):
    return pl.pallas_call(
        kernel,
        out_shape=outs,
        in_specs=[SMEM] * scalars + [VMEM] * (len(ins) - scalars),
        out_specs=jax.tree.map(lambda _: VMEM, outs),
        scratch_shapes=list(scratch),
        compiler_params=pltpu.CompilerParams(vmem_limit_bytes=mib << 20),
    )(*ins)


def to_all(value, axis, copies):
    return lax.all_to_all(
        jnp.broadcast_to(value, (copies, *value.shape)), axis, 0, 0, tiled=True
    )


def rotate_kernel(at, *refs):
    *pieces, out = refs
    count = len(pieces)
    for k in range(count):
        slot = lax.rem(at[0] + count - k, count)
        out[:, pl.ds(slot, 1)] = pieces[k][...][:, None]


def placed(pieces, at):
    lead, *rest = pieces[0].shape
    out = jax.ShapeDtypeStruct((lead, len(pieces), *rest), pieces[0].dtype)
    return local_call(rotate_kernel, out, (at, *pieces), 1, mib=8)


def around(value, axis):
    count = lax.axis_size(axis)
    return [value] + [lax.ppermute(value, axis, cycle(count, k)) for k in range(1, count)]


def norm_kernel(at, gain, tail, *refs):
    *pieces, out = refs
    count = len(pieces)
    rows = pieces[0].shape[0]

    def normed(values):
        values = values.astype(F32)
        mean = jnp.mean(values * values, axis=-1, keepdims=True)
        return (values * lax.rsqrt(mean + EPS) * gain[...]).astype(BF16)

    out[count * rows :, :] = normed(tail[...])
    for k in range(count):
        first = lax.rem(at[0] + count - k, count) * rows

        def chunk(r, carry):
            to = pl.multiple_of(first + r * 16, 16)
            out[pl.ds(to, 16), :] = normed(pieces[k][pl.ds(pl.multiple_of(r * 16, 16), 16), :])
            return carry

        lax.fori_loop(0, rows // 16, chunk, 0, unroll=5)


def scan_kernel(
    core, own, other, step, rate, taps, y_out, c_out, reach_out, state_out, rows_seq, buf, state, offset
):
    length = step.shape[0]
    inner = y_out.shape[1] // 2
    heads = inner // HEAD_DIM
    rows_seq[pl.ds(core[0], 1)] = own[...][None]
    rows_seq[pl.ds(1 - core[0], 1)] = other[...][None]
    buf[:, 0:8, :] = rows_seq[:, length + 8 : length + 16, :].astype(F32)
    state[...] = jnp.zeros_like(state)
    offset[...] = jnp.zeros_like(offset)
    causal = lax.broadcasted_iota(jnp.int32, (BLOCK, BLOCK), 0) >= lax.broadcasted_iota(
        jnp.int32, (BLOCK, BLOCK), 1
    )
    lower = causal.astype(F32)

    def block(i, carry):
        here = pl.ds(i * BLOCK, BLOCK)
        steps = step[here, :]
        cum = jnp.dot(
            lower, -steps * rate[...], precision=lax.Precision.HIGHEST, preferred_element_type=F32
        )
        cum_t = cum.T
        total = cum[BLOCK - 1 : BLOCK, :]
        decay = jnp.exp(cum)
        tail_weight = jnp.exp(total - cum)
        total_decay = jnp.exp(total)
        reach_out[here, :] = jnp.exp(cum + offset[...])
        offset[...] = offset[...] + total
        for g in range(2):
            buf[g, 8 : 8 + BLOCK, :] = rows_seq[g, here, :].astype(F32)
            summed = taps[g, 0:1, :] * buf[g, 5 : 5 + BLOCK, :]
            for k in range(1, CONV):
                summed = summed + taps[g, k : k + 1, :] * buf[g, 5 + k : 5 + k + BLOCK, :]
            buf[g, 0:8, :] = buf[g, BLOCK : BLOCK + 8, :]
            mixed = silu(summed)
            xs = mixed[:, :inner]
            bs = mixed[:, inner : inner + STATE]
            cs = mixed[:, inner + STATE :].astype(BF16)
            scores = lax.dot_general(
                cs, bs.astype(BF16), (((1,), (1,)), ((), ())), preferred_element_type=F32
            )
            old = state[g]
            reached = jnp.dot(cs, old.astype(BF16), preferred_element_type=F32)
            tails, factors, ys = [], [], []
            for h in range(heads):
                cut = slice(h * HEAD_DIM, (h + 1) * HEAD_DIM)
                lane = slice(g * heads + h, g * heads + h + 1)
                scaled = xs[:, cut] * steps[:, lane]
                gap = cum[:, lane] - cum_t[lane, :]
                within = jnp.where(causal, jnp.exp(jnp.where(causal, gap, 0.0)), 0.0) * scores
                inside = jnp.dot(
                    within.astype(BF16), scaled.astype(BF16), preferred_element_type=F32
                )
                ys.append(inside + reached[:, cut] * decay[:, lane])
                tails.append(scaled * tail_weight[:, lane])
                factors.append(jnp.broadcast_to(total_decay[:, lane], (1, HEAD_DIM)))
            y_out[here, g * inner : (g + 1) * inner] = jnp.concatenate(ys, axis=1)
            c_out[here, g * STATE : (g + 1) * STATE] = cs
            fresh = jnp.dot(
                bs.T.astype(BF16),
                jnp.concatenate(tails, axis=1).astype(BF16),
                preferred_element_type=F32,
            )
            state[g] = old * jnp.concatenate(factors, axis=1) + fresh
        return carry

    lax.fori_loop(0, length // BLOCK, block, 0)
    share = STATE // state_out.shape[0]
    for part in range(state_out.shape[0]):
        rows = slice(part * share, (part + 1) * share)
        write_packed(
            state_out,
            part,
            jnp.concatenate([state[0, rows, :], state[1, rows, :]], axis=1),
            jnp.exp(offset[...]),
        )


def write_packed(out, part, states, factor):
    width = states.shape[1]
    high = factor.astype(BF16).astype(F32)
    low = factor - high
    pick = lax.broadcasted_iota(jnp.int32, (states.shape[0], factor.shape[1]), 0)
    extra = jnp.where(pick == 0, high, jnp.where(pick == 1, low, 0.0))
    out[part, :, 0:width] = states.astype(BF16)
    out[part, :, width:] = extra.astype(BF16)


def read_packed(ref, part):
    width = ref.shape[2] - 128
    extra = ref[part, :, width:].astype(F32)
    return extra[0:1, :] + extra[1:2, :], ref[part, :, 0:width].astype(F32)


def widened(factor, width):
    return jnp.concatenate(
        [
            jnp.broadcast_to(factor[:, h : h + 1], (factor.shape[0], HEAD_DIM))
            for h in range(width // HEAD_DIM)
        ],
        axis=1,
    )


def plane_kernel(pieces, out):
    factor, states = read_packed(pieces, 0)
    for k in range(1, pieces.shape[0]):
        next_factor, next_states = read_packed(pieces, k)
        states = states * widened(next_factor, states.shape[1]) + next_states
        factor = factor * next_factor
    for k in range(out.shape[0]):
        write_packed(out, k, states, factor)


def enter_kernel(at, pieces, planes, out):
    run = jnp.zeros(out.shape[1:], F32)
    for k in range(planes.shape[0]):
        factor, states = read_packed(planes, k)
        run = jnp.where(k < at[0], run * widened(factor, run.shape[1]) + states, run)
    for k in range(pieces.shape[0]):
        out[k] = run.astype(BF16)
        factor, states = read_packed(pieces, k)
        run = run * widened(factor, run.shape[1]) + states


def gate_kernel(core, y, cs, reach, entering, gate_own, gate_other, gain, out):
    inner = y.shape[1] // 2
    heads = inner // HEAD_DIM

    def block(i, carry):
        here = pl.ds(pl.multiple_of(i * BLOCK, BLOCK), BLOCK)
        weight = reach[here, :]
        own, other = (gate[here, :].astype(F32) for gate in (gate_own, gate_other))
        for g in range(2):
            cut = slice(g * inner, (g + 1) * inner)
            reached = jnp.dot(
                cs[here, g * STATE : (g + 1) * STATE],
                entering[:, cut],
                preferred_element_type=F32,
            )
            expanded = widened(weight[:, g * heads : (g + 1) * heads], inner)
            gates = jnp.where(core[0] == g, own, other)
            gated = (y[here, cut] + reached * expanded) * silu(gates)
            mean = jnp.mean(gated * gated, axis=-1, keepdims=True)
            out[here, cut] = (gated * lax.rsqrt(mean + EPS) * gain[:, cut]).astype(BF16)
        return carry

    lax.fori_loop(0, y.shape[0] // BLOCK, block, 0)


def dot(a, b):
    return jnp.dot(a, b, preferred_element_type=F32)


def dot_t(a, b):
    return lax.dot_general(a, b, (((1,), (1,)), ((), ())), preferred_element_type=F32)


def body(
    tokens, in_gain, w_x, w_z, w_b, w_c, w_dt, conv_x, conv_b, conv_c, dt_bias, a_log, out_gain, w_out
):
    x_at, c_at, y_at, z_at = (lax.axis_index(a) for a in ("x", "c", "y", "z"))
    x_one, c_one, y_one, z_one = (v.reshape(1) for v in (x_at, c_at, y_at, z_at))
    n_z, n_x, n_y = (lax.axis_size(a) for a in ("z", "x", "y"))
    rows, width = tokens.shape
    length = rows * n_y
    inner = w_x.shape[1] // 2
    state = w_b.shape[1] // 2
    heads = 2 * inner // HEAD_DIM
    cut = inner + 2 * state
    core_swap = cycle(2, 1)

    def halves_swapped(*arrays):
        def columns_of(core):
            return jnp.concatenate(
                [
                    lax.dynamic_slice_in_dim(w, core * (w.shape[1] // 2), w.shape[1] // 2, 1)
                    for w in arrays
                ],
                axis=1,
            )

        mine = columns_of(c_at)
        swapped = lax.ppermute(columns_of(1 - c_at), "c", core_swap)
        return jnp.where(
            c_at == 0,
            jnp.concatenate([mine, swapped], axis=0),
            jnp.concatenate([swapped, mine], axis=0),
        )

    first_source = halves_swapped(w_x, w_b, w_c)
    pieces = around(tokens, "y")
    first_z = to_all(first_source, "z", n_z)

    def here(v, size):
        return lax.dynamic_slice_in_dim(v, y_at * size, size, v.ndim - 1)

    lanes = 128
    dt_weight = jnp.pad(here(w_dt, heads), ((0, 0), (0, lanes - heads)))
    bias = jnp.pad(here(dt_bias, heads), (0, lanes - heads))
    rate = jnp.pad(jnp.exp(here(a_log, heads)), (0, lanes - heads)).reshape(1, lanes)
    taps = jnp.concatenate(
        [
            here(v, 2 * size).reshape(CONV, 2, size).swapaxes(0, 1)
            for v, size in ((conv_x, inner), (conv_b, state), (conv_c, state))
        ],
        axis=2,
    )
    gain = here(out_gain, 2 * inner).reshape(1, -1)
    first_z, taps, rate, bias, dt_weight, gain = lax.optimization_barrier(
        (first_z, taps, rate, bias, dt_weight, gain)
    )
    first_pieces = around(first_z, "x")
    second_source = halves_swapped(w_z, w_out.T)
    second_source, first_z = lax.optimization_barrier((second_source, first_z))
    second_z = to_all(second_source, "z", n_z)

    ends = lax.select_n(lax.rem(y_at + 1, n_y), *(piece[rows - 16 :] for piece in pieces))
    chain_steps = [(a, a + 1) for a in range(2 * n_z * n_x - 1)]
    tail = lax.ppermute(ends, ("z", "x", "c"), chain_steps)
    normed = local_call(
        norm_kernel,
        jax.ShapeDtypeStruct((length + 16, width), BF16),
        (y_one, in_gain.reshape(1, -1), tail, *pieces),
        1,
    )

    step = jax.nn.softplus(dot(normed[:length], dt_weight) + bias)
    first_pieces, step = lax.optimization_barrier((first_pieces, step))
    first = placed(first_pieces, x_one).reshape(width, cut)
    first_other = lax.ppermute(first, "c", core_swap)
    proj = [dot(normed, w).astype(BF16) for w in (first, first_other)]
    parts = 2 * n_x
    share = STATE // parts
    y_local, c_rows, reach, final = local_call(
        scan_kernel,
        (
            jax.ShapeDtypeStruct((length, 2 * inner), F32),
            jax.ShapeDtypeStruct((length, 2 * STATE), BF16),
            jax.ShapeDtypeStruct((length, lanes), F32),
            jax.ShapeDtypeStruct((parts, share, 2 * inner + lanes), BF16),
        ),
        (c_one, *proj, step, rate, taps),
        1,
        (
            pltpu.VMEM((2, length + 16, cut), BF16),
            pltpu.VMEM((2, BLOCK + 8, cut), F32),
            pltpu.VMEM((2, STATE, inner), F32),
            pltpu.VMEM((1, lanes), F32),
        ),
    )

    final, second_z = lax.optimization_barrier((final, second_z))
    second_pieces = around(second_z, "x")
    second = placed(second_pieces, x_one).reshape(width, 2 * inner)
    second_other = lax.ppermute(second, "c", core_swap)

    within_plane = lax.all_to_all(final, ("x", "c"), 0, 0, tiled=True)
    sent = local_call(
        plane_kernel, jax.ShapeDtypeStruct((n_z, share, 2 * inner + lanes), BF16), (within_plane,)
    )
    planes = lax.all_to_all(sent, "z", 0, 0, tiled=True)
    back = local_call(
        enter_kernel,
        jax.ShapeDtypeStruct((parts, share, 2 * inner), BF16),
        (z_one, within_plane, planes),
        1,
    )
    entering = lax.all_to_all(back, ("x", "c"), 0, 0, tiled=True).reshape(STATE, 2 * inner)

    gates = [dot(normed[:length], w[:, :inner]).astype(BF16) for w in (second, second_other)]
    halves = [w[:, inner:] for w in (second, second_other)]
    out_weight = jnp.where(
        c_at == 0, jnp.concatenate(halves, axis=1), jnp.concatenate(halves[::-1], axis=1)
    )
    mixed = local_call(
        gate_kernel,
        jax.ShapeDtypeStruct((length, 2 * inner), BF16),
        (c_one, y_local, c_rows, reach, entering, *gates, gain),
        1,
    )

    partial = dot_t(mixed, out_weight).astype(BF16).reshape(n_y, rows, width)
    shares = lax.all_to_all(partial, "y", 0, 0, tiled=True)
    return jnp.sum(shares.astype(F32), axis=0).astype(BF16)


def solution(mesh):
    split = Mesh(mesh.devices.reshape(16, 4, 2, mesh.shape["tp"]), ALL)
    sp = ("z", "x", "c")
    in_specs = (
        P(ALL, None), P(), P(sp, "y"), P(sp, "y"), P(sp, "y"), P(sp, "y"),
        P(), P(), P(), P(), P(), P(), P(), P("y", sp),
    )
    return jax.shard_map(
        body, mesh=split, in_specs=in_specs, out_specs=P(ALL, None), check_vma=False
    )
```

```python
import jax
import jax.numpy as jnp
from jax import lax
from jax.experimental import pallas as pl
from jax.experimental.pallas import tpu as pltpu
from jax.sharding import Mesh
from jax.sharding import PartitionSpec as P

HEAD_DIM = 64
STATE = 128
CONV = 4
BLOCK = 128
EPS = 1e-06
F32 = jnp.float32
BF16 = jnp.bfloat16
ALL = ("z", "x", "c", "y")


SMEM = pl.BlockSpec(memory_space=pltpu.SMEM)
VMEM = pl.BlockSpec(memory_space=pltpu.VMEM)


def cycle(count, step):
    return [(a, (a + step) % count) for a in range(count)]


def silu(v):
    return v / (1.0 + jnp.exp(-v))


def local_call(kernel, outs, ins, scalars=0, scratch=(), mib=16):
    return pl.pallas_call(
        kernel,
        out_shape=outs,
        in_specs=[SMEM] * scalars + [VMEM] * (len(ins) - scalars),
        out_specs=jax.tree.map(lambda _: VMEM, outs),
        scratch_shapes=list(scratch),
        compiler_params=pltpu.CompilerParams(vmem_limit_bytes=mib << 20),
    )(*ins)


def rotate_kernel(at, *refs):
    *pieces, out = refs
    count = len(pieces)
    for k in range(count):
        slot = lax.rem(at[0] + count - k, count)
        out[:, pl.ds(slot, 1)] = pieces[k][...][:, None]


def placed(pieces, at):
    lead, *rest = pieces[0].shape
    out = jax.ShapeDtypeStruct((lead, len(pieces), *rest), pieces[0].dtype)
    return local_call(rotate_kernel, out, (at, *pieces), 1, mib=8)


def around(value, axis):
    count = lax.axis_size(axis)
    return [value] + [lax.ppermute(value, axis, cycle(count, k)) for k in range(1, count)]


def norm_kernel(at, gain, tail, *refs):
    *pieces, out = refs
    count = len(pieces)
    rows = pieces[0].shape[0]

    def normed(values):
        values = values.astype(F32)
        mean = jnp.mean(values * values, axis=-1, keepdims=True)
        return (values * lax.rsqrt(mean + EPS) * gain[...]).astype(BF16)

    out[count * rows :, :] = normed(tail[...])
    for k in range(count):
        first = lax.rem(at[0] + count - k, count) * rows

        def chunk(r, carry):
            to = pl.multiple_of(first + r * 16, 16)
            out[pl.ds(to, 16), :] = normed(pieces[k][pl.ds(pl.multiple_of(r * 16, 16), 16), :])
            return carry

        lax.fori_loop(0, rows // 16, chunk, 0, unroll=5)


def scan_kernel(
    core, own, other, step, rate, taps, y_out, c_out, reach_out, state_out, rows_seq, buf, state, offset
):
    length = step.shape[0]
    inner = y_out.shape[1] // 2
    heads = inner // HEAD_DIM
    rows_seq[pl.ds(core[0], 1)] = own[...][None]
    rows_seq[pl.ds(1 - core[0], 1)] = other[...][None]
    buf[:, 0:8, :] = rows_seq[:, length + 8 : length + 16, :].astype(F32)
    state[...] = jnp.zeros_like(state)
    offset[...] = jnp.zeros_like(offset)
    causal = lax.broadcasted_iota(jnp.int32, (BLOCK, BLOCK), 0) >= lax.broadcasted_iota(
        jnp.int32, (BLOCK, BLOCK), 1
    )
    lower = causal.astype(F32)

    def block(i, carry):
        here = pl.ds(i * BLOCK, BLOCK)
        steps = step[here, :]
        cum = jnp.dot(
            lower, -steps * rate[...], precision=lax.Precision.HIGHEST, preferred_element_type=F32
        )
        cum_t = cum.T
        total = cum[BLOCK - 1 : BLOCK, :]
        decay = jnp.exp(cum)
        tail_weight = jnp.exp(total - cum)
        total_decay = jnp.exp(total)
        reach_out[here, :] = jnp.exp(cum + offset[...])
        offset[...] = offset[...] + total
        for g in range(2):
            buf[g, 8 : 8 + BLOCK, :] = rows_seq[g, here, :].astype(F32)
            summed = taps[g, 0:1, :] * buf[g, 5 : 5 + BLOCK, :]
            for k in range(1, CONV):
                summed = summed + taps[g, k : k + 1, :] * buf[g, 5 + k : 5 + k + BLOCK, :]
            buf[g, 0:8, :] = buf[g, BLOCK : BLOCK + 8, :]
            mixed = silu(summed)
            xs = mixed[:, :inner]
            bs = mixed[:, inner : inner + STATE]
            cs = mixed[:, inner + STATE :].astype(BF16)
            scores = lax.dot_general(
                cs, bs.astype(BF16), (((1,), (1,)), ((), ())), preferred_element_type=F32
            )
            old = state[g]
            reached = jnp.dot(cs, old.astype(BF16), preferred_element_type=F32)
            tails, factors, ys = [], [], []
            for h in range(heads):
                cut = slice(h * HEAD_DIM, (h + 1) * HEAD_DIM)
                lane = slice(g * heads + h, g * heads + h + 1)
                scaled = xs[:, cut] * steps[:, lane]
                gap = cum[:, lane] - cum_t[lane, :]
                within = jnp.where(causal, jnp.exp(jnp.where(causal, gap, 0.0)), 0.0) * scores
                inside = jnp.dot(
                    within.astype(BF16), scaled.astype(BF16), preferred_element_type=F32
                )
                ys.append(inside + reached[:, cut] * decay[:, lane])
                tails.append(scaled * tail_weight[:, lane])
                factors.append(jnp.broadcast_to(total_decay[:, lane], (1, HEAD_DIM)))
            y_out[here, g * inner : (g + 1) * inner] = jnp.concatenate(ys, axis=1)
            c_out[here, g * STATE : (g + 1) * STATE] = cs
            fresh = jnp.dot(
                bs.T.astype(BF16),
                jnp.concatenate(tails, axis=1).astype(BF16),
                preferred_element_type=F32,
            )
            state[g] = old * jnp.concatenate(factors, axis=1) + fresh
        return carry

    lax.fori_loop(0, length // BLOCK, block, 0)
    share = STATE // state_out.shape[0]
    for part in range(state_out.shape[0]):
        rows = slice(part * share, (part + 1) * share)
        write_packed(
            state_out,
            part,
            jnp.concatenate([state[0, rows, :], state[1, rows, :]], axis=1),
            jnp.exp(offset[...]),
        )


def write_packed(out, part, states, factor):
    width = states.shape[1]
    high = factor.astype(BF16).astype(F32)
    low = factor - high
    pick = lax.broadcasted_iota(jnp.int32, (states.shape[0], factor.shape[1]), 0)
    extra = jnp.where(pick == 0, high, jnp.where(pick == 1, low, 0.0))
    out[part, :, 0:width] = states.astype(BF16)
    out[part, :, width:] = extra.astype(BF16)


def read_packed(ref, part):
    width = ref.shape[2] - 128
    extra = ref[part, :, width:].astype(F32)
    return extra[0:1, :] + extra[1:2, :], ref[part, :, 0:width].astype(F32)


def widened(factor, width):
    return jnp.concatenate(
        [
            jnp.broadcast_to(factor[:, h : h + 1], (factor.shape[0], HEAD_DIM))
            for h in range(width // HEAD_DIM)
        ],
        axis=1,
    )


def plane_kernel(pieces, out):
    factor, states = read_packed(pieces, 0)
    for k in range(1, pieces.shape[0]):
        next_factor, next_states = read_packed(pieces, k)
        states = states * widened(next_factor, states.shape[1]) + next_states
        factor = factor * next_factor
    for k in range(out.shape[0]):
        write_packed(out, k, states, factor)


def enter_kernel(at, pieces, planes, out):
    run = jnp.zeros(out.shape[1:], F32)
    for k in range(planes.shape[0]):
        factor, states = read_packed(planes, k)
        run = jnp.where(k < at[0], run * widened(factor, run.shape[1]) + states, run)
    for k in range(pieces.shape[0]):
        out[k] = run.astype(BF16)
        factor, states = read_packed(pieces, k)
        run = run * widened(factor, run.shape[1]) + states


def gate_kernel(core, y, cs, reach, entering, gate_own, gate_other, gain, out):
    inner = y.shape[1] // 2
    heads = inner // HEAD_DIM

    def block(i, carry):
        here = pl.ds(pl.multiple_of(i * BLOCK, BLOCK), BLOCK)
        weight = reach[here, :]
        own, other = (gate[here, :].astype(F32) for gate in (gate_own, gate_other))
        for g in range(2):
            cut = slice(g * inner, (g + 1) * inner)
            reached = jnp.dot(
                cs[here, g * STATE : (g + 1) * STATE],
                entering[:, cut],
                preferred_element_type=F32,
            )
            expanded = widened(weight[:, g * heads : (g + 1) * heads], inner)
            gates = jnp.where(core[0] == g, own, other)
            gated = (y[here, cut] + reached * expanded) * silu(gates)
            mean = jnp.mean(gated * gated, axis=-1, keepdims=True)
            out[here, cut] = (gated * lax.rsqrt(mean + EPS) * gain[:, cut]).astype(BF16)
        return carry

    lax.fori_loop(0, y.shape[0] // BLOCK, block, 0)


def dot(a, b):
    return jnp.dot(a, b, preferred_element_type=F32)


def dot_t(a, b):
    return lax.dot_general(a, b, (((1,), (1,)), ((), ())), preferred_element_type=F32)


def body(
    tokens, in_gain, w_x, w_z, w_b, w_c, w_dt, conv_x, conv_b, conv_c, dt_bias, a_log, out_gain, w_out
):
    x_at, c_at, y_at, z_at = (lax.axis_index(a) for a in ("x", "c", "y", "z"))
    x_one, c_one, y_one, z_one = (v.reshape(1) for v in (x_at, c_at, y_at, z_at))
    n_z, n_x, n_y = (lax.axis_size(a) for a in ("z", "x", "y"))
    rows, width = tokens.shape
    length = rows * n_y
    inner = w_x.shape[1] // 2
    state = w_b.shape[1] // 2
    heads = 2 * inner // HEAD_DIM
    cut = inner + 2 * state
    core_swap = cycle(2, 1)

    def halves(*arrays):
        parts = [a.reshape(a.shape[0], 2, -1).swapaxes(0, 1) for a in arrays]
        return jnp.concatenate(parts, axis=2)

    def along_z(source):
        sent = jnp.broadcast_to(source, (n_z, *source.shape)).reshape(-1, *source.shape[1:])
        got = lax.all_to_all(sent, ("z", "c"), 0, 0, tiled=True)
        return got.reshape(n_z, -1, got.shape[-1])

    first_source = halves(w_x, w_b, w_c)
    pieces = around(tokens, "y")
    first_z = along_z(first_source)

    def here(v, size):
        return lax.dynamic_slice_in_dim(v, y_at * size, size, v.ndim - 1)

    lanes = 128
    dt_weight = jnp.pad(here(w_dt, heads), ((0, 0), (0, lanes - heads)))
    bias = jnp.pad(here(dt_bias, heads), (0, lanes - heads))
    rate = jnp.pad(jnp.exp(here(a_log, heads)), (0, lanes - heads)).reshape(1, lanes)
    taps = jnp.concatenate(
        [
            here(v, 2 * size).reshape(CONV, 2, size).swapaxes(0, 1)
            for v, size in ((conv_x, inner), (conv_b, state), (conv_c, state))
        ],
        axis=2,
    )
    gain = here(out_gain, 2 * inner).reshape(1, -1)
    first_z, taps, rate, bias, dt_weight, gain = lax.optimization_barrier(
        (first_z, taps, rate, bias, dt_weight, gain)
    )
    first_pieces = around(first_z, "x")
    second_source = halves(w_z, w_out.T)
    second_source, first_z = lax.optimization_barrier((second_source, first_z))
    second_z = along_z(second_source)

    ends = lax.select_n(lax.rem(y_at + 1, n_y), *(piece[rows - 16 :] for piece in pieces))
    chain_steps = [(a, a + 1) for a in range(2 * n_z * n_x - 1)]
    tail = lax.ppermute(ends, ("z", "x", "c"), chain_steps)
    normed = local_call(
        norm_kernel,
        jax.ShapeDtypeStruct((length + 16, width), BF16),
        (y_one, in_gain.reshape(1, -1), tail, *pieces),
        1,
    )

    step = jax.nn.softplus(dot(normed[:length], dt_weight) + bias)
    first_pieces, step = lax.optimization_barrier((first_pieces, step))
    first = placed(first_pieces, x_one).reshape(width, cut)
    first_other = lax.ppermute(first, "c", core_swap)
    proj = [dot(normed, w).astype(BF16) for w in (first, first_other)]
    parts = 2 * n_x
    share = STATE // parts
    y_local, c_rows, reach, final = local_call(
        scan_kernel,
        (
            jax.ShapeDtypeStruct((length, 2 * inner), F32),
            jax.ShapeDtypeStruct((length, 2 * STATE), BF16),
            jax.ShapeDtypeStruct((length, lanes), F32),
            jax.ShapeDtypeStruct((parts, share, 2 * inner + lanes), BF16),
        ),
        (c_one, *proj, step, rate, taps),
        1,
        (
            pltpu.VMEM((2, length + 16, cut), BF16),
            pltpu.VMEM((2, BLOCK + 8, cut), F32),
            pltpu.VMEM((2, STATE, inner), F32),
            pltpu.VMEM((1, lanes), F32),
        ),
    )

    final, second_z = lax.optimization_barrier((final, second_z))
    second_pieces = around(second_z, "x")
    second = placed(second_pieces, x_one).reshape(width, 2 * inner)
    second_other = lax.ppermute(second, "c", core_swap)

    within_plane = lax.all_to_all(final, ("x", "c"), 0, 0, tiled=True)
    sent = local_call(
        plane_kernel, jax.ShapeDtypeStruct((n_z, share, 2 * inner + lanes), BF16), (within_plane,)
    )
    planes = lax.all_to_all(sent, "z", 0, 0, tiled=True)
    back = local_call(
        enter_kernel,
        jax.ShapeDtypeStruct((parts, share, 2 * inner), BF16),
        (z_one, within_plane, planes),
        1,
    )
    entering = lax.all_to_all(back, ("x", "c"), 0, 0, tiled=True).reshape(STATE, 2 * inner)

    gates = [dot(normed[:length], second[:, :inner]).astype(BF16)]
    gates.append(dot(normed[:length], second_other[:, :inner]).astype(BF16))
    ends = [w[:, inner:] for w in (second, second_other)]
    out_weight = jnp.where(
        c_at == 0, jnp.concatenate(ends, axis=1), jnp.concatenate(ends[::-1], axis=1)
    )
    out_weight, entering = lax.optimization_barrier((out_weight, entering))
    mixed = local_call(
        gate_kernel,
        jax.ShapeDtypeStruct((length, 2 * inner), BF16),
        (c_one, y_local, c_rows, reach, entering, *gates, gain),
        1,
    )

    partial = dot_t(mixed, out_weight).astype(BF16).reshape(n_y, rows, width)
    shares = lax.all_to_all(partial, "y", 0, 0, tiled=True)
    return jnp.sum(shares.astype(F32), axis=0).astype(BF16)


def solution(mesh):
    split = Mesh(mesh.devices.reshape(16, 4, 2, mesh.shape["tp"]), ALL)
    sp = ("z", "x", "c")
    in_specs = (
        P(ALL, None), P(), P(sp, "y"), P(sp, "y"), P(sp, "y"), P(sp, "y"),
        P(), P(), P(), P(), P(), P(), P(), P("y", sp),
    )
    return jax.shard_map(
        body, mesh=split, in_specs=in_specs, out_specs=P(ALL, None), check_vma=False
    )
```

```python
import jax
import jax.numpy as jnp
from jax import lax
from jax.experimental import pallas as pl
from jax.experimental.pallas import tpu as pltpu
from jax.sharding import Mesh
from jax.sharding import PartitionSpec as P

HEAD_DIM = 64
STATE = 128
CONV = 4
BLOCK = 128
EPS = 1e-06
F32 = jnp.float32
BF16 = jnp.bfloat16
ALL = ("z", "x", "c", "y")


SMEM = pl.BlockSpec(memory_space=pltpu.SMEM)
VMEM = pl.BlockSpec(memory_space=pltpu.VMEM)


def cycle(count, step):
    return [(a, (a + step) % count) for a in range(count)]


def silu(v):
    return v / (1.0 + jnp.exp(-v))


def local_call(kernel, outs, ins, scalars=0, scratch=(), mib=16):
    return pl.pallas_call(
        kernel,
        out_shape=outs,
        in_specs=[SMEM] * scalars + [VMEM] * (len(ins) - scalars),
        out_specs=jax.tree.map(lambda _: VMEM, outs),
        scratch_shapes=list(scratch),
        compiler_params=pltpu.CompilerParams(vmem_limit_bytes=mib << 20),
    )(*ins)


def to_all(value, axis, copies):
    return lax.all_to_all(
        jnp.broadcast_to(value, (copies, *value.shape)), axis, 0, 0, tiled=True
    )


def rotate_kernel(at, *refs):
    *pieces, out = refs
    count = len(pieces)
    for k in range(count):
        slot = lax.rem(at[0] + count - k, count)
        out[:, pl.ds(slot, 1)] = pieces[k][...][:, None]


def placed(pieces, at):
    lead, *rest = pieces[0].shape
    out = jax.ShapeDtypeStruct((lead, len(pieces), *rest), pieces[0].dtype)
    return local_call(rotate_kernel, out, (at, *pieces), 1, mib=8)


def around(value, axis):
    count = lax.axis_size(axis)
    return [value] + [lax.ppermute(value, axis, cycle(count, k)) for k in range(1, count)]


def norm_kernel(at, gain, tail, *refs):
    *pieces, out = refs
    count = len(pieces)
    rows = pieces[0].shape[0]

    def normed(values):
        values = values.astype(F32)
        mean = jnp.mean(values * values, axis=-1, keepdims=True)
        return (values * lax.rsqrt(mean + EPS) * gain[...]).astype(BF16)

    out[count * rows :, :] = normed(tail[...])
    for k in range(count):
        first = lax.rem(at[0] + count - k, count) * rows

        def chunk(r, carry):
            to = pl.multiple_of(first + r * 16, 16)
            out[pl.ds(to, 16), :] = normed(pieces[k][pl.ds(pl.multiple_of(r * 16, 16), 16), :])
            return carry

        lax.fori_loop(0, rows // 16, chunk, 0, unroll=5)


def scan_kernel(
    core, own, other, step, rate, taps, y_out, c_out, reach_out, state_out, rows_seq, buf, state, offset
):
    length = step.shape[0]
    inner = y_out.shape[1] // 2
    heads = inner // HEAD_DIM
    rows_seq[pl.ds(core[0], 1)] = own[...][None]
    rows_seq[pl.ds(1 - core[0], 1)] = other[...][None]
    buf[:, 0:8, :] = rows_seq[:, length + 8 : length + 16, :].astype(F32)
    state[...] = jnp.zeros_like(state)
    offset[...] = jnp.zeros_like(offset)
    causal = lax.broadcasted_iota(jnp.int32, (BLOCK, BLOCK), 0) >= lax.broadcasted_iota(
        jnp.int32, (BLOCK, BLOCK), 1
    )
    lower = causal.astype(F32)

    def block(i, carry):
        here = pl.ds(i * BLOCK, BLOCK)
        steps = step[here, :]
        cum = jnp.dot(
            lower, -steps * rate[...], precision=lax.Precision.HIGHEST, preferred_element_type=F32
        )
        cum_t = cum.T
        total = cum[BLOCK - 1 : BLOCK, :]
        decay = jnp.exp(cum)
        tail_weight = jnp.exp(total - cum)
        total_decay = jnp.exp(total)
        reach_out[here, :] = jnp.exp(cum + offset[...])
        offset[...] = offset[...] + total
        for g in range(2):
            buf[g, 8 : 8 + BLOCK, :] = rows_seq[g, here, :].astype(F32)
            window = buf[g]
            summed = taps[g, CONV - 1 : CONV, :] * window[8:, :]
            for k in range(CONV - 1):
                behind = pltpu.roll(window, CONV - 1 - k, 0)
                summed = summed + taps[g, k : k + 1, :] * behind[8:, :]
            buf[g, 0:8, :] = buf[g, BLOCK : BLOCK + 8, :]
            mixed = silu(summed)
            xs = mixed[:, :inner]
            bs = mixed[:, inner : inner + STATE]
            cs = mixed[:, inner + STATE :].astype(BF16)
            scores = lax.dot_general(
                cs, bs.astype(BF16), (((1,), (1,)), ((), ())), preferred_element_type=F32
            )
            old = state[g]
            reached = jnp.dot(cs, old.astype(BF16), preferred_element_type=F32)
            tails, factors, ys = [], [], []
            for h in range(heads):
                cut = slice(h * HEAD_DIM, (h + 1) * HEAD_DIM)
                lane = slice(g * heads + h, g * heads + h + 1)
                scaled = xs[:, cut] * steps[:, lane]
                gap = cum[:, lane] - cum_t[lane, :]
                within = jnp.exp(jnp.where(causal, gap, -jnp.inf)) * scores
                inside = jnp.dot(
                    within.astype(BF16), scaled.astype(BF16), preferred_element_type=F32
                )
                ys.append(inside + reached[:, cut] * decay[:, lane])
                tails.append(scaled * tail_weight[:, lane])
                factors.append(jnp.broadcast_to(total_decay[:, lane], (1, HEAD_DIM)))
            y_out[here, g * inner : (g + 1) * inner] = jnp.concatenate(ys, axis=1)
            c_out[here, g * STATE : (g + 1) * STATE] = cs
            fresh = jnp.dot(
                bs.T.astype(BF16),
                jnp.concatenate(tails, axis=1).astype(BF16),
                preferred_element_type=F32,
            )
            state[g] = old * jnp.concatenate(factors, axis=1) + fresh
        return carry

    lax.fori_loop(0, length // BLOCK, block, 0)
    share = STATE // state_out.shape[0]
    for part in range(state_out.shape[0]):
        rows = slice(part * share, (part + 1) * share)
        write_packed(
            state_out,
            part,
            jnp.concatenate([state[0, rows, :], state[1, rows, :]], axis=1),
            jnp.exp(offset[...]),
        )


def write_packed(out, part, states, factor):
    width = states.shape[1]
    high = factor.astype(BF16).astype(F32)
    low = factor - high
    pick = lax.broadcasted_iota(jnp.int32, (states.shape[0], factor.shape[1]), 0)
    extra = jnp.where(pick == 0, high, jnp.where(pick == 1, low, 0.0))
    out[part, :, 0:width] = states.astype(BF16)
    out[part, :, width:] = extra.astype(BF16)


def read_packed(ref, part):
    width = ref.shape[2] - 128
    extra = ref[part, :, width:].astype(F32)
    return extra[0:1, :] + extra[1:2, :], ref[part, :, 0:width].astype(F32)


def widened(factor, width):
    return jnp.concatenate(
        [
            jnp.broadcast_to(factor[:, h : h + 1], (factor.shape[0], HEAD_DIM))
            for h in range(width // HEAD_DIM)
        ],
        axis=1,
    )


def plane_kernel(pieces, out):
    factor, states = read_packed(pieces, 0)
    for k in range(1, pieces.shape[0]):
        next_factor, next_states = read_packed(pieces, k)
        states = states * widened(next_factor, states.shape[1]) + next_states
        factor = factor * next_factor
    for k in range(out.shape[0]):
        write_packed(out, k, states, factor)


def enter_kernel(at, pieces, planes, out):
    run = jnp.zeros(out.shape[1:], F32)
    for k in range(planes.shape[0]):
        factor, states = read_packed(planes, k)
        run = jnp.where(k < at[0], run * widened(factor, run.shape[1]) + states, run)
    for k in range(pieces.shape[0]):
        out[k] = run.astype(BF16)
        factor, states = read_packed(pieces, k)
        run = run * widened(factor, run.shape[1]) + states


def gate_kernel(core, y, cs, reach, entering, gate_own, gate_other, gain, out):
    inner = y.shape[1] // 2
    heads = inner // HEAD_DIM

    def block(i, carry):
        here = pl.ds(pl.multiple_of(i * BLOCK, BLOCK), BLOCK)
        weight = reach[here, :]
        own, other = (gate[here, :].astype(F32) for gate in (gate_own, gate_other))
        for g in range(2):
            cut = slice(g * inner, (g + 1) * inner)
            reached = jnp.dot(
                cs[here, g * STATE : (g + 1) * STATE],
                entering[:, cut],
                preferred_element_type=F32,
            )
            expanded = widened(weight[:, g * heads : (g + 1) * heads], inner)
            gates = jnp.where(core[0] == g, own, other)
            gated = (y[here, cut] + reached * expanded) * silu(gates)
            mean = jnp.mean(gated * gated, axis=-1, keepdims=True)
            out[here, cut] = (gated * lax.rsqrt(mean + EPS) * gain[:, cut]).astype(BF16)
        return carry

    lax.fori_loop(0, y.shape[0] // BLOCK, block, 0)


def dot(a, b):
    return jnp.dot(a, b, preferred_element_type=F32)


def dot_t(a, b):
    return lax.dot_general(a, b, (((1,), (1,)), ((), ())), preferred_element_type=F32)


def body(
    tokens, in_gain, w_x, w_z, w_b, w_c, w_dt, conv_x, conv_b, conv_c, dt_bias, a_log, out_gain, w_out
):
    x_at, c_at, y_at, z_at = (lax.axis_index(a) for a in ("x", "c", "y", "z"))
    x_one, c_one, y_one, z_one = (v.reshape(1) for v in (x_at, c_at, y_at, z_at))
    n_z, n_x, n_y = (lax.axis_size(a) for a in ("z", "x", "y"))
    rows, width = tokens.shape
    length = rows * n_y
    inner = w_x.shape[1] // 2
    state = w_b.shape[1] // 2
    heads = 2 * inner // HEAD_DIM
    cut = inner + 2 * state
    core_swap = cycle(2, 1)

    def halves_swapped(*arrays):
        def columns_of(core):
            return jnp.concatenate(
                [
                    lax.dynamic_slice_in_dim(w, core * (w.shape[1] // 2), w.shape[1] // 2, 1)
                    for w in arrays
                ],
                axis=1,
            )

        mine = columns_of(c_at)
        swapped = lax.ppermute(columns_of(1 - c_at), "c", core_swap)
        return jnp.where(
            c_at == 0,
            jnp.concatenate([mine, swapped], axis=0),
            jnp.concatenate([swapped, mine], axis=0),
        )

    first_source = halves_swapped(w_x, w_b, w_c)
    pieces = around(tokens, "y")
    first_z = to_all(first_source, "z", n_z)

    def here(v, size):
        return lax.dynamic_slice_in_dim(v, y_at * size, size, v.ndim - 1)

    lanes = 128
    dt_weight = jnp.pad(here(w_dt, heads), ((0, 0), (0, lanes - heads)))
    bias = jnp.pad(here(dt_bias, heads), (0, lanes - heads))
    rate = jnp.pad(jnp.exp(here(a_log, heads)), (0, lanes - heads)).reshape(1, lanes)
    taps = jnp.concatenate(
        [
            here(v, 2 * size).reshape(CONV, 2, size).swapaxes(0, 1)
            for v, size in ((conv_x, inner), (conv_b, state), (conv_c, state))
        ],
        axis=2,
    )
    gain = here(out_gain, 2 * inner).reshape(1, -1)
    first_z, taps, rate, bias, dt_weight, gain = lax.optimization_barrier(
        (first_z, taps, rate, bias, dt_weight, gain)
    )
    first_pieces = around(first_z, "x")
    second_source = halves_swapped(w_z, w_out.T)
    second_source, first_z = lax.optimization_barrier((second_source, first_z))
    second_z = to_all(second_source, "z", n_z)

    ends = lax.select_n(lax.rem(y_at + 1, n_y), *(piece[rows - 16 :] for piece in pieces))
    chain_steps = [(a, a + 1) for a in range(2 * n_z * n_x - 1)]
    tail = lax.ppermute(ends, ("z", "x", "c"), chain_steps)
    normed = local_call(
        norm_kernel,
        jax.ShapeDtypeStruct((length + 16, width), BF16),
        (y_one, in_gain.reshape(1, -1), tail, *pieces),
        1,
    )

    step = jax.nn.softplus(dot(normed[:length], dt_weight) + bias)
    first_pieces, step = lax.optimization_barrier((first_pieces, step))
    first = placed(first_pieces, x_one).reshape(width, cut)
    first_other = lax.ppermute(first, "c", core_swap)
    proj = [dot(normed, w).astype(BF16) for w in (first, first_other)]
    parts = 2 * n_x
    share = STATE // parts
    y_local, c_rows, reach, final = local_call(
        scan_kernel,
        (
            jax.ShapeDtypeStruct((length, 2 * inner), F32),
            jax.ShapeDtypeStruct((length, 2 * STATE), BF16),
            jax.ShapeDtypeStruct((length, lanes), F32),
            jax.ShapeDtypeStruct((parts, share, 2 * inner + lanes), BF16),
        ),
        (c_one, *proj, step, rate, taps),
        1,
        (
            pltpu.VMEM((2, length + 16, cut), BF16),
            pltpu.VMEM((2, BLOCK + 8, cut), F32),
            pltpu.VMEM((2, STATE, inner), F32),
            pltpu.VMEM((1, lanes), F32),
        ),
    )

    final, second_z = lax.optimization_barrier((final, second_z))
    second_pieces = around(second_z, "x")
    second = placed(second_pieces, x_one).reshape(width, 2 * inner)
    second_other = lax.ppermute(second, "c", core_swap)

    within_plane = lax.all_to_all(final, ("x", "c"), 0, 0, tiled=True)
    sent = local_call(
        plane_kernel, jax.ShapeDtypeStruct((n_z, share, 2 * inner + lanes), BF16), (within_plane,)
    )
    planes = lax.all_to_all(sent, "z", 0, 0, tiled=True)
    back = local_call(
        enter_kernel,
        jax.ShapeDtypeStruct((parts, share, 2 * inner), BF16),
        (z_one, within_plane, planes),
        1,
    )
    entering = lax.all_to_all(back, ("x", "c"), 0, 0, tiled=True).reshape(STATE, 2 * inner)

    gates = [dot(normed[:length], second[:, :inner]).astype(BF16)]
    gates.append(dot(normed[:length], second_other[:, :inner]).astype(BF16))
    ends = [w[:, inner:] for w in (second, second_other)]
    out_weight = jnp.where(
        c_at == 0, jnp.concatenate(ends, axis=1), jnp.concatenate(ends[::-1], axis=1)
    )
    out_weight, entering = lax.optimization_barrier((out_weight, entering))
    mixed = local_call(
        gate_kernel,
        jax.ShapeDtypeStruct((length, 2 * inner), BF16),
        (c_one, y_local, c_rows, reach, entering, *gates, gain),
        1,
    )

    partial = dot_t(mixed, out_weight).astype(BF16).reshape(n_y, rows, width)
    shares = lax.all_to_all(partial, "y", 0, 0, tiled=True)
    return jnp.sum(shares.astype(F32), axis=0).astype(BF16)


def solution(mesh):
    split = Mesh(mesh.devices.reshape(16, 4, 2, mesh.shape["tp"]), ALL)
    sp = ("z", "x", "c")
    in_specs = (
        P(ALL, None), P(), P(sp, "y"), P(sp, "y"), P(sp, "y"), P(sp, "y"),
        P(), P(), P(), P(), P(), P(), P(), P("y", sp),
    )
    return jax.shard_map(
        body, mesh=split, in_specs=in_specs, out_specs=P(ALL, None), check_vma=False
    )
```

```python
import jax
import jax.numpy as jnp
from jax import lax
from jax.experimental import pallas as pl
from jax.experimental.pallas import tpu as pltpu
from jax.sharding import Mesh
from jax.sharding import PartitionSpec as P

HEAD_DIM = 64
STATE = 128
CONV = 4
BLOCK = 128
EPS = 1e-06
F32 = jnp.float32
BF16 = jnp.bfloat16
ALL = ("z", "x", "c", "y")


SMEM = pl.BlockSpec(memory_space=pltpu.SMEM)
VMEM = pl.BlockSpec(memory_space=pltpu.VMEM)


def cycle(count, step):
    return [(a, (a + step) % count) for a in range(count)]


def silu(v):
    return v / (1.0 + jnp.exp(-v))


def local_call(kernel, outs, ins, scalars=0, scratch=(), mib=16):
    return pl.pallas_call(
        kernel,
        out_shape=outs,
        in_specs=[SMEM] * scalars + [VMEM] * (len(ins) - scalars),
        out_specs=jax.tree.map(lambda _: VMEM, outs),
        scratch_shapes=list(scratch),
        compiler_params=pltpu.CompilerParams(vmem_limit_bytes=mib << 20),
    )(*ins)


def to_all(value, axis, copies):
    return lax.all_to_all(
        jnp.broadcast_to(value, (copies, *value.shape)), axis, 0, 0, tiled=True
    )


def rotate_kernel(at, *refs):
    *pieces, out = refs
    count = len(pieces)
    for k in range(count):
        slot = lax.rem(at[0] + count - k, count)
        out[:, pl.ds(slot, 1)] = pieces[k][...][:, None]


def placed(pieces, at):
    lead, *rest = pieces[0].shape
    out = jax.ShapeDtypeStruct((lead, len(pieces), *rest), pieces[0].dtype)
    return local_call(rotate_kernel, out, (at, *pieces), 1, mib=8)


def around(value, axis):
    count = lax.axis_size(axis)
    return [value] + [lax.ppermute(value, axis, cycle(count, k)) for k in range(1, count)]


def norm_kernel(at, gain, tail, *refs):
    *pieces, out = refs
    count = len(pieces)
    rows = pieces[0].shape[0]

    def normed(values):
        values = values.astype(F32)
        mean = jnp.mean(values * values, axis=-1, keepdims=True)
        return (values * lax.rsqrt(mean + EPS) * gain[...]).astype(BF16)

    out[count * rows :, :] = normed(tail[...])
    for k in range(count):
        first = lax.rem(at[0] + count - k, count) * rows

        def chunk(r, carry):
            to = pl.multiple_of(first + r * 16, 16)
            out[pl.ds(to, 16), :] = normed(pieces[k][pl.ds(pl.multiple_of(r * 16, 16), 16), :])
            return carry

        lax.fori_loop(0, rows // 16, chunk, 0, unroll=5)


def scan_kernel(
    core, own, other, step, rate, taps, rows_out, reach_out, state_out, rows_seq, buf, state, offset
):
    length = step.shape[0]
    inner = state.shape[2]
    heads = inner // HEAD_DIM
    rows_seq[pl.ds(core[0], 1)] = own[...][None]
    rows_seq[pl.ds(1 - core[0], 1)] = other[...][None]
    buf[:, 0:8, :] = rows_seq[:, length + 8 : length + 16, :].astype(F32)
    state[...] = jnp.zeros_like(state)
    offset[...] = jnp.zeros_like(offset)
    causal = lax.broadcasted_iota(jnp.int32, (BLOCK, BLOCK), 0) >= lax.broadcasted_iota(
        jnp.int32, (BLOCK, BLOCK), 1
    )
    lower = causal.astype(F32)

    def block(i, carry):
        here = pl.ds(i * BLOCK, BLOCK)
        steps = step[here, :]
        cum = jnp.dot(
            lower, -steps * rate[...], precision=lax.Precision.HIGHEST, preferred_element_type=F32
        )
        cum_t = cum.T
        total = cum[BLOCK - 1 : BLOCK, :]
        decay = jnp.exp(cum)
        tail_weight = jnp.exp(total - cum)
        total_decay = jnp.exp(total)
        reach_out[here, :] = jnp.exp(cum + offset[...])
        offset[...] = offset[...] + total
        for g in range(2):
            buf[g, 8 : 8 + BLOCK, :] = rows_seq[g, here, :].astype(F32)
            window = buf[g]
            summed = taps[g, CONV - 1 : CONV, :] * window[8:, :]
            for k in range(CONV - 1):
                behind = pltpu.roll(window, CONV - 1 - k, 0)
                summed = summed + taps[g, k : k + 1, :] * behind[8:, :]
            buf[g, 0:8, :] = buf[g, BLOCK : BLOCK + 8, :]
            mixed = silu(summed)
            xs = mixed[:, :inner]
            bs = mixed[:, inner : inner + STATE]
            cs = mixed[:, inner + STATE :].astype(BF16)
            scores = lax.dot_general(
                cs, bs.astype(BF16), (((1,), (1,)), ((), ())), preferred_element_type=F32
            )
            old = state[g]
            reached = jnp.dot(cs, old.astype(BF16), preferred_element_type=F32)
            tails, factors, ys = [], [], []
            for h in range(heads):
                cut = slice(h * HEAD_DIM, (h + 1) * HEAD_DIM)
                lane = slice(g * heads + h, g * heads + h + 1)
                scaled = xs[:, cut] * steps[:, lane]
                gap = cum[:, lane] - cum_t[lane, :]
                within = jnp.exp(jnp.where(causal, gap, -jnp.inf)) * scores
                inside = jnp.dot(
                    within.astype(BF16), scaled.astype(BF16), preferred_element_type=F32
                )
                ys.append(inside + reached[:, cut] * decay[:, lane])
                tails.append(scaled * tail_weight[:, lane])
                factors.append(jnp.broadcast_to(total_decay[:, lane], (1, HEAD_DIM)))
            rows_out[here, g * inner : (g + 1) * inner] = jnp.concatenate(ys, axis=1).astype(BF16)
            rows_out[here, 2 * inner + g * STATE : 2 * inner + (g + 1) * STATE] = cs
            fresh = jnp.dot(
                bs.T.astype(BF16),
                jnp.concatenate(tails, axis=1).astype(BF16),
                preferred_element_type=F32,
            )
            state[g] = old * jnp.concatenate(factors, axis=1) + fresh
        return carry

    lax.fori_loop(0, length // BLOCK, block, 0)
    share = STATE // state_out.shape[0]
    for part in range(state_out.shape[0]):
        rows = slice(part * share, (part + 1) * share)
        write_packed(
            state_out,
            part,
            jnp.concatenate([state[0, rows, :], state[1, rows, :]], axis=1),
            jnp.exp(offset[...]),
        )


def write_packed(out, part, states, factor):
    width = states.shape[1]
    high = factor.astype(BF16).astype(F32)
    low = factor - high
    pick = lax.broadcasted_iota(jnp.int32, (states.shape[0], factor.shape[1]), 0)
    extra = jnp.where(pick == 0, high, jnp.where(pick == 1, low, 0.0))
    out[part, :, 0:width] = states.astype(BF16)
    out[part, :, width:] = extra.astype(BF16)


def read_packed(ref, part):
    width = ref.shape[2] - 128
    extra = ref[part, :, width:].astype(F32)
    return extra[0:1, :] + extra[1:2, :], ref[part, :, 0:width].astype(F32)


def widened(factor, width):
    return jnp.concatenate(
        [
            jnp.broadcast_to(factor[:, h : h + 1], (factor.shape[0], HEAD_DIM))
            for h in range(width // HEAD_DIM)
        ],
        axis=1,
    )


def plane_kernel(pieces, out):
    factor, states = read_packed(pieces, 0)
    for k in range(1, pieces.shape[0]):
        next_factor, next_states = read_packed(pieces, k)
        states = states * widened(next_factor, states.shape[1]) + next_states
        factor = factor * next_factor
    for k in range(out.shape[0]):
        write_packed(out, k, states, factor)


def enter_kernel(at, pieces, planes, out):
    run = jnp.zeros(out.shape[1:], F32)
    for k in range(planes.shape[0]):
        factor, states = read_packed(planes, k)
        run = jnp.where(k < at[0], run * widened(factor, run.shape[1]) + states, run)
    for k in range(pieces.shape[0]):
        out[k] = run.astype(BF16)
        factor, states = read_packed(pieces, k)
        run = run * widened(factor, run.shape[1]) + states


def gate_kernel(core, local, reach, entering, gate_own, gate_other, gain, out):
    inner = entering.shape[1] // 2
    heads = inner // HEAD_DIM

    def block(i, carry):
        here = pl.ds(pl.multiple_of(i * BLOCK, BLOCK), BLOCK)
        weight = reach[here, :]
        own, other = (gate[here, :].astype(F32) for gate in (gate_own, gate_other))
        for g in range(2):
            cut = slice(g * inner, (g + 1) * inner)
            reached = jnp.dot(
                local[here, 2 * inner + g * STATE : 2 * inner + (g + 1) * STATE],
                entering[:, cut],
                preferred_element_type=F32,
            )
            expanded = widened(weight[:, g * heads : (g + 1) * heads], inner)
            gates = jnp.where(core[0] == g, own, other)
            gated = (local[here, cut].astype(F32) + reached * expanded) * silu(gates)
            mean = jnp.mean(gated * gated, axis=-1, keepdims=True)
            out[here, cut] = (gated * lax.rsqrt(mean + EPS) * gain[:, cut]).astype(BF16)
        return carry

    lax.fori_loop(0, local.shape[0] // BLOCK, block, 0)


def dot(a, b):
    return jnp.dot(a, b, preferred_element_type=F32)


def dot_t(a, b):
    return lax.dot_general(a, b, (((1,), (1,)), ((), ())), preferred_element_type=F32)


def body(
    tokens, in_gain, w_x, w_z, w_b, w_c, w_dt, conv_x, conv_b, conv_c, dt_bias, a_log, out_gain, w_out
):
    x_at, c_at, y_at, z_at = (lax.axis_index(a) for a in ("x", "c", "y", "z"))
    x_one, c_one, y_one, z_one = (v.reshape(1) for v in (x_at, c_at, y_at, z_at))
    n_z, n_x, n_y = (lax.axis_size(a) for a in ("z", "x", "y"))
    rows, width = tokens.shape
    length = rows * n_y
    inner = w_x.shape[1] // 2
    state = w_b.shape[1] // 2
    heads = 2 * inner // HEAD_DIM
    cut = inner + 2 * state
    core_swap = cycle(2, 1)

    def halves_swapped(*arrays):
        def columns_of(core):
            return jnp.concatenate(
                [
                    lax.dynamic_slice_in_dim(w, core * (w.shape[1] // 2), w.shape[1] // 2, 1)
                    for w in arrays
                ],
                axis=1,
            )

        mine = columns_of(c_at)
        swapped = lax.ppermute(columns_of(1 - c_at), "c", core_swap)
        return jnp.where(
            c_at == 0,
            jnp.concatenate([mine, swapped], axis=0),
            jnp.concatenate([swapped, mine], axis=0),
        )

    first_source = halves_swapped(w_x, w_b, w_c)
    pieces = around(tokens, "y")
    first_z = to_all(first_source, "z", n_z)

    def here(v, size):
        return lax.dynamic_slice_in_dim(v, y_at * size, size, v.ndim - 1)

    lanes = 128
    dt_weight = jnp.pad(here(w_dt, heads), ((0, 0), (0, lanes - heads)))
    bias = jnp.pad(here(dt_bias, heads), (0, lanes - heads))
    rate = jnp.pad(jnp.exp(here(a_log, heads)), (0, lanes - heads)).reshape(1, lanes)
    taps = jnp.concatenate(
        [
            here(v, 2 * size).reshape(CONV, 2, size).swapaxes(0, 1)
            for v, size in ((conv_x, inner), (conv_b, state), (conv_c, state))
        ],
        axis=2,
    )
    gain = here(out_gain, 2 * inner).reshape(1, -1)
    first_z, taps, rate, bias, dt_weight, gain = lax.optimization_barrier(
        (first_z, taps, rate, bias, dt_weight, gain)
    )
    first_pieces = around(first_z, "x")
    second_source = halves_swapped(w_z, w_out.T)
    second_source, first_z = lax.optimization_barrier((second_source, first_z))
    second_z = to_all(second_source, "z", n_z)

    ends = lax.select_n(lax.rem(y_at + 1, n_y), *(piece[rows - 16 :] for piece in pieces))
    chain_steps = [(a, a + 1) for a in range(2 * n_z * n_x - 1)]
    tail = lax.ppermute(ends, ("z", "x", "c"), chain_steps)
    normed = local_call(
        norm_kernel,
        jax.ShapeDtypeStruct((length + 16, width), BF16),
        (y_one, in_gain.reshape(1, -1), tail, *pieces),
        1,
    )

    step = jax.nn.softplus(dot(normed[:length], dt_weight) + bias)
    first_pieces, step = lax.optimization_barrier((first_pieces, step))
    first = placed(first_pieces, x_one).reshape(width, cut)
    first_other = lax.ppermute(first, "c", core_swap)
    proj = [dot(normed, w).astype(BF16) for w in (first, first_other)]
    parts = 2 * n_x
    share = STATE // parts
    local, reach, final = local_call(
        scan_kernel,
        (
            jax.ShapeDtypeStruct((length, 2 * inner + 2 * STATE), BF16),
            jax.ShapeDtypeStruct((length, lanes), F32),
            jax.ShapeDtypeStruct((parts, share, 2 * inner + lanes), BF16),
        ),
        (c_one, *proj, step, rate, taps),
        1,
        (
            pltpu.VMEM((2, length + 16, cut), BF16),
            pltpu.VMEM((2, BLOCK + 8, cut), F32),
            pltpu.VMEM((2, STATE, inner), F32),
            pltpu.VMEM((1, lanes), F32),
        ),
    )

    final, second_z = lax.optimization_barrier((final, second_z))
    second_pieces = around(second_z, "x")
    second = placed(second_pieces, x_one).reshape(width, 2 * inner)
    second_other = lax.ppermute(second, "c", core_swap)

    within_plane = lax.all_to_all(final, ("x", "c"), 0, 0, tiled=True)
    sent = local_call(
        plane_kernel, jax.ShapeDtypeStruct((n_z, share, 2 * inner + lanes), BF16), (within_plane,)
    )
    planes = lax.all_to_all(sent, "z", 0, 0, tiled=True)
    back = local_call(
        enter_kernel,
        jax.ShapeDtypeStruct((parts, share, 2 * inner), BF16),
        (z_one, within_plane, planes),
        1,
    )
    entering = lax.all_to_all(back, ("x", "c"), 0, 0, tiled=True).reshape(STATE, 2 * inner)

    gates = [dot(normed[:length], second[:, :inner]).astype(BF16)]
    gates.append(dot(normed[:length], second_other[:, :inner]).astype(BF16))
    ends = [w[:, inner:] for w in (second, second_other)]
    out_weight = jnp.where(
        c_at == 0, jnp.concatenate(ends, axis=1), jnp.concatenate(ends[::-1], axis=1)
    )
    out_weight, entering = lax.optimization_barrier((out_weight, entering))
    mixed = local_call(
        gate_kernel,
        jax.ShapeDtypeStruct((length, 2 * inner), BF16),
        (c_one, local, reach, entering, *gates, gain),
        1,
    )

    partial = dot_t(mixed, out_weight).astype(BF16).reshape(n_y, rows, width)
    shares = lax.all_to_all(partial, "y", 0, 0, tiled=True)
    return jnp.sum(shares.astype(F32), axis=0).astype(BF16)


def solution(mesh):
    split = Mesh(mesh.devices.reshape(16, 4, 2, mesh.shape["tp"]), ALL)
    sp = ("z", "x", "c")
    in_specs = (
        P(ALL, None), P(), P(sp, "y"), P(sp, "y"), P(sp, "y"), P(sp, "y"),
        P(), P(), P(), P(), P(), P(), P(), P("y", sp),
    )
    return jax.shard_map(
        body, mesh=split, in_specs=in_specs, out_specs=P(ALL, None), check_vma=False
    )
```
